256 devices in a mesh: grp: 2 (over z), ep: 64 (over y, x), tp: 2 (over core).
Axes of the slice: x: 8, y: 8, z: 2, core: 2. Of those that a mesh axis runs over, the one named last changes fastest.
The devices are a block of a 8x8x16 slice.
Arguments:
- tokens: bfloat16 [65536, 2048], P(('grp', 'ep'), 'tp'), parts along dimension 0, may hold values from -6 to 6
- norm_gain: float32 [2048], replicated, may hold values from 0.1 to 1.9
- expert_ids: int32 [65536, 2], P(('grp', 'ep')), parts along dimension 0, may hold values from 0 to 63, all different within a row; in each aligned block of 512 rows (0 to 511, 512 to 1023, ...) at most 24 rows name the same one
- route_weights: float32 [65536, 2], P(('grp', 'ep')), parts along dimension 0, may hold values from 0.1 to 1
- gate_weight: bfloat16 [64, 2048, 512], P('ep', None, 'tp'), may hold values from -0.125 to 0.125
- up_weight: bfloat16 [64, 2048, 512], P('ep', None, 'tp'), may hold values from -0.125 to 0.125
- down_weight: bfloat16 [64, 512, 2048], P('ep', None, 'tp'), may hold values from -0.25 to 0.25
Outputs:
- mixed: bfloat16 [65536, 2048], P(('grp', 'ep'), 'tp'), parts along dimension 0
The draws below stay inside these ranges and needn't reach their ends.
There are 2 independent parts, one for each index of `grp`. The reference program is written for one: setup_inputs(seed, part) draws one part's arguments, and reference() takes and returns one part's arrays. A program takes and returns all parts, laid end to end along the dimension named above; an argument that names none is the same for every part. Nothing has to cross between parts.
Inputs may be any that keep to these rules, and one draw needn't show every extreme that they name: `expert_ids`: each token names 2 different experts. Among the 512 tokens of one index of ep (aligned blocks of rows) at most 24 name the same expert, and in some block some expert is named by exactly 24 of them.
All inputs are finite; a program needn't handle non-finite values.
Results may differ from the reference program's by a relative error of at most 0.007.
Values may be sent and summed in bfloat16 or wider, within the bound.
No kernel may reach another device: no remote copies, remote signals or barrier semaphores. Data moves between devices by JAX's collectives and lax.ppermute only.
A program may use at most 64 MiB of HBM per device.

```python
import math
import jax
import jax.numpy as jnp
import numpy as np
from jax import lax

D = 2048
DE = 512
TOP_K = 2
TOK_DEV = 512
EXPERTS = 64
TOKENS = 32768
CAP = 24
N_EP = 64


def levels(key, dims, pieces, least, high):
    def one(dim, parts):
        draws = jax.random.uniform(jax.random.fold_in(jax.random.fold_in(key, 6), dim), (parts,), jnp.float32, least / len(pieces), high / len(pieces))
        return jnp.repeat(jnp.exp(draws), dims[dim] // parts).reshape((-1,) + (1,) * (len(dims) - dim - 1))

    factor_of = one(*pieces[0])
    for cut in pieces[1:]:
        factor_of = factor_of * one(*cut)
    return factor_of


def shared_out(own_key, own, number, rows, amount, top, bound, lean):
    sequence = jax.random.permutation(own_key, amount)
    crowded, ordinary = shares(amount, rows * top, bound, lean, True), shares(amount, rows * top, bound, lean, False)
    places = jnp.arange(amount)

    def named(lengths, turn):
        used = int((lengths > 0).sum())
        fixed = max(1, used // 4)
        passed = fixed + (places - fixed + turn * (used - fixed)) % max(1, amount - fixed)
        return jnp.zeros((amount,), jnp.int32).at[sequence[jnp.where(places < fixed, places, passed)]].set(jnp.asarray(lengths, jnp.int32))

    lengths = jnp.where(number % 4 == 0, named(crowded, number // 4), named(ordinary, number - number // 4 - 1))
    mixed = jax.random.permutation(jax.random.fold_in(own, 3), amount)
    giver, receiver = mixed[0:amount // 2 * 2:2], mixed[1:amount // 2 * 2:2]
    room = jnp.minimum(lengths[giver] - 1, bound - lengths[receiver]) // 2
    room = jnp.where((giver == sequence[0]) | (receiver == sequence[0]) | (lengths[receiver] == 0), 0, jnp.maximum(room, 0))
    passed = jax.random.randint(jax.random.fold_in(own, 4), (amount // 2,), 0, 1 << 20) % (room + 1)
    lengths = lengths.at[giver].add(-passed).at[receiver].add(passed)
    labels = jnp.searchsorted(jnp.cumsum(lengths), jnp.arange(rows * top), side="right").astype(jnp.int32)
    table = labels.reshape(top, rows).T
    table = table[jax.random.permutation(jax.random.fold_in(own, 1), rows)]
    turn = jax.random.randint(jax.random.fold_in(own, 2), (rows, 1), 0, top)
    return jnp.take_along_axis(table, (jnp.arange(top)[None, :] + turn) % top, axis=1)


def shares(amount, total, bound, lean, full):
    portions = [(1 << 20) // math.isqrt(grade ** lean) + 1 for grade in range(1, amount + 1)]
    largest = bound if full else min(bound, max(-(-total // amount), total * portions[0] // sum(portions)))
    least = 1 if total - largest >= amount - 1 else 0
    counts, surplus = [largest] + [least] * (amount - 1), total - largest - least * (amount - 1)
    while surplus > 0:
        free = [i for i in range(1, amount) if counts[i] < largest] or [i for i in range(1, amount) if counts[i] < bound]
        whole, remaining = sum([portions[i] for i in free]), surplus
        for i in free:
            extra = min(bound - counts[i], max(1, remaining * portions[i] // whole), surplus)
            counts[i] = counts[i] + extra
            surplus = surplus - extra
    return np.array(counts)


def gaussian(own_key, extent, scale, limit, split=(), kind=jnp.bfloat16):
    entries = scale * jax.random.normal(own_key, extent, jnp.float32)
    if split:
        entries = entries * levels(own_key, extent, split, -0.22, 0.18)
    return jnp.clip(entries, -limit, limit).astype(kind)


def setup_inputs(seed: int = 0, part: int = 0) -> dict:
    key_of = jax.random.split(jax.random.key(seed), 8)
    own_keys = jax.random.split(jax.random.fold_in(key_of[7], part), 8)
    tokens = gaussian(own_keys[0], (TOKENS, D), 1.0, 6.0, ((0, 64), (1, 2)))
    norm_gain = jnp.clip(1.0 + 0.18 * jax.random.normal(key_of[1], (D,), jnp.float32), 0.1, 1.9)
    expert_ids_keys = jax.random.split(jax.random.fold_in(own_keys[2], 1), TOKENS // TOK_DEV)
    expert_ids_turns = jax.random.permutation(jax.random.fold_in(own_keys[2], 3), TOKENS // TOK_DEV)
    expert_ids = jax.vmap(lambda own, number: shared_out(jax.random.fold_in(own_keys[2], 2), own, number, TOK_DEV, EXPERTS, TOP_K, CAP, 2))(expert_ids_keys, expert_ids_turns).reshape((TOKENS, TOP_K))
    route_weights = jnp.clip(jnp.exp(math.log(1.0) - 2.3025851 * jax.random.uniform(own_keys[3], (TOKENS, TOP_K), jnp.float32) ** levels(own_keys[3], (TOKENS, TOP_K), ((0, 64),), -0.2, 0.2)), 0.1, 1.0)
    gate_weight = gaussian(key_of[4], (EXPERTS, D, DE), D ** -0.5, 0.125, ((0, 64), (2, 2)))
    up_weight = gaussian(key_of[5], (EXPERTS, D, DE), D ** -0.5, 0.125, ((0, 64), (2, 2)))
    down_weight = gaussian(key_of[6], (EXPERTS, DE, D), DE ** -0.5, 0.25, ((0, 64), (2, 2)))
    return dict(tokens=tokens, norm_gain=norm_gain, expert_ids=expert_ids, route_weights=route_weights, gate_weight=gate_weight, up_weight=up_weight, down_weight=down_weight)


def reference(tokens, norm_gain, expert_ids, route_weights, gate_weight, up_weight, down_weight):
    xf = tokens.astype(jnp.float32)
    scale = lax.rsqrt(lax.optimization_barrier(jnp.mean(xf * xf, axis=-1, keepdims=True)) + 1e-06)
    normed = (xf * scale * norm_gain.astype(jnp.float32)[None, :]).astype(jnp.bfloat16)
    flat = expert_ids.reshape(-1).astype(jnp.int32)
    pairs = flat.shape[0]
    onehot = (flat[:, None] == jnp.arange(EXPERTS, dtype=jnp.int32)[None, :]).astype(jnp.int32)
    blocked = onehot.reshape(-1, TOK_DEV * TOP_K, EXPERTS)
    earlier = (jnp.cumsum(blocked, axis=1) - blocked).reshape(pairs, EXPERTS)
    slot = lax.optimization_barrier(jnp.sum(earlier * onehot, axis=-1)).astype(jnp.int32)
    block = (jnp.arange(pairs, dtype=jnp.int32) // (TOK_DEV * TOP_K)).astype(jnp.int32)
    position = (block * CAP + slot).astype(jnp.int32)
    owner = (jnp.arange(pairs, dtype=jnp.int32) // TOP_K).astype(jnp.int32)
    source = jnp.full((EXPERTS, N_EP * CAP), TOKENS, jnp.int32).at[flat, position].set(owner)
    weights = jnp.zeros((EXPERTS, N_EP * CAP), jnp.float32).at[flat, position].set(route_weights.reshape(-1).astype(jnp.float32))
    padded = jnp.concatenate([normed, jnp.zeros((1, normed.shape[1]), jnp.bfloat16)], axis=0)

    def one_expert(total, inputs):
        rows_idx, row_w, w_gate, w_up, w_down = inputs
        rows = padded[rows_idx]
        gate = jnp.dot(rows, w_gate, preferred_element_type=jnp.float32)
        upper = jnp.dot(rows, w_up, preferred_element_type=jnp.float32)
        hidden = (jax.nn.silu(gate) * upper).astype(jnp.bfloat16)
        result = jnp.dot(hidden, w_down, preferred_element_type=jnp.float32).astype(jnp.bfloat16)
        total = total.at[rows_idx].add(result.astype(jnp.float32) * row_w[:, None])
        return (total, None)
    start = jnp.zeros((TOKENS + 1, normed.shape[1]), jnp.float32)
    total, _ = lax.scan(one_expert, start, (source, weights, gate_weight, up_weight, down_weight))
    return total[:TOKENS].astype(jnp.bfloat16)
```

```python
import jax
import jax.numpy as jnp
from jax import lax
from jax.experimental import pallas as pl
from jax.experimental.pallas import tpu as pltpu
from jax.sharding import PartitionSpec as P

CHUNKS = ((0, 24),)
BF16 = jnp.bfloat16
F32 = jnp.float32


def block_of(total, most):
    size = most
    while total % size:
        size -= 8
    return size


def strictly_before(n, rows_earlier):
    row = lax.broadcasted_iota(jnp.int32, (n, n), 0)
    col = lax.broadcasted_iota(jnp.int32, (n, n), 1)
    earlier = row < col if rows_earlier else col < row
    return jnp.where(earlier, 1.0, 0.0).astype(BF16)


def select_rows(ids_t, tokens, experts, first, count):
    tok, half = tokens.shape
    per = block_of(experts, 16)

    def kernel(ids_ref, tok_ref, out_ref, key_ref):
        step = pl.program_id(0)

        @pl.when(step == 0)
        def _():
            expert = lax.broadcasted_iota(jnp.int32, (experts, tok), 0)
            named = (ids_ref[0:1, :] == expert) | (ids_ref[1:2, :] == expert)
            named_f = jnp.where(named, 1.0, 0.0)
            slot = jnp.dot(named_f.astype(BF16), strictly_before(tok, True), preferred_element_type=F32)
            key_ref[...] = jnp.where(named, slot, -1.0)

        key = key_ref[pl.ds(pl.multiple_of(step * per, per), per), :]
        wanted = (lax.broadcasted_iota(jnp.int32, (per, count, tok), 1) + first).astype(F32)
        chosen = jnp.where(key[:, None, :] == wanted, 1.0, 0.0).reshape(per * count, tok).astype(BF16)
        out_ref[...] = jnp.dot(chosen, tok_ref[...], preferred_element_type=F32).astype(BF16)

    return pl.pallas_call(
        kernel,
        grid=(experts // per,),
        in_specs=[
            pl.BlockSpec((2, tok), lambda i: (0, 0)),
            pl.BlockSpec((tok, half), lambda i: (0, 0)),
        ],
        out_specs=pl.BlockSpec((per * count, half), lambda i: (i, 0)),
        out_shape=jax.ShapeDtypeStruct((experts * count, half), BF16),
        scratch_shapes=[pltpu.VMEM((experts, tok), F32)],
        cost_estimate=pl.CostEstimate(
            flops=2 * experts * count * tok * half, bytes_accessed=2 * (tok + experts * count) * half, transcendentals=0
        ),
        name="select_rows",
    )(ids_t, tokens)


def hidden_units(core, own, other, gain, w_gate, w_up):
    rows, half = own.shape
    units = w_gate.shape[1]
    block = block_of(rows, 256)

    def kernel(core_ref, own_ref, other_ref, gain_a, gain_b, wg_a, wg_b, wu_a, wu_b, out_ref):
        a = own_ref[...].astype(F32)
        b = other_ref[...].astype(F32)
        total = jnp.sum(a * a, axis=-1, keepdims=True) + jnp.sum(b * b, axis=-1, keepdims=True)
        scale = lax.rsqrt(total * (1.0 / (2 * half)) + 1e-06)
        na = (a * scale * gain_a[0]).astype(BF16)
        nb = (b * scale * gain_b[0]).astype(BF16)
        gate = jnp.dot(na, wg_a[0], preferred_element_type=F32) + jnp.dot(nb, wg_b[0], preferred_element_type=F32)
        upper = jnp.dot(na, wu_a[0], preferred_element_type=F32) + jnp.dot(nb, wu_b[0], preferred_element_type=F32)
        out_ref[...] = (gate / (1.0 + jnp.exp(-gate)) * upper).astype(BF16)

    mine = lambda i, c: (c[0], 0, 0)
    theirs = lambda i, c: (1 - c[0], 0, 0)
    w_gate = w_gate.reshape(2, half, units)
    w_up = w_up.reshape(2, half, units)
    gain = gain.reshape(2, 1, half)
    return pl.pallas_call(
        kernel,
        grid_spec=pltpu.PrefetchScalarGridSpec(
            num_scalar_prefetch=1,
            grid=(rows // block,),
            in_specs=[
                pl.BlockSpec((block, half), lambda i, c: (i, 0)),
                pl.BlockSpec((block, half), lambda i, c: (i, 0)),
                pl.BlockSpec((1, 1, half), mine),
                pl.BlockSpec((1, 1, half), theirs),
                pl.BlockSpec((1, half, units), mine),
                pl.BlockSpec((1, half, units), theirs),
                pl.BlockSpec((1, half, units), mine),
                pl.BlockSpec((1, half, units), theirs),
            ],
            out_specs=pl.BlockSpec((block, units), lambda i, c: (i, 0)),
        ),
        out_shape=jax.ShapeDtypeStruct((rows, units), BF16),
        cost_estimate=pl.CostEstimate(
            flops=8 * rows * half * units, bytes_accessed=4 * rows * half, transcendentals=rows * units
        ),
        name="hidden_units",
    )(core, own, other, gain, gain, w_gate, w_gate, w_up, w_up)


def down_rows(core, own, other, w_down):
    rows, units = own.shape
    half = w_down.shape[1]
    block = block_of(rows, 256)

    def kernel(core_ref, own_ref, other_ref, w_a, w_b, out_ref):
        out = jnp.dot(own_ref[...], w_a[0], preferred_element_type=F32)
        out = out + jnp.dot(other_ref[...], w_b[0], preferred_element_type=F32)
        out_ref[...] = out.astype(BF16)

    w_down = w_down.reshape(2, units, half)
    return pl.pallas_call(
        kernel,
        grid_spec=pltpu.PrefetchScalarGridSpec(
            num_scalar_prefetch=1,
            grid=(rows // block,),
            in_specs=[
                pl.BlockSpec((block, units), lambda i, c: (i, 0)),
                pl.BlockSpec((block, units), lambda i, c: (i, 0)),
                pl.BlockSpec((1, units, half), lambda i, c: (c[0], 0, 0)),
                pl.BlockSpec((1, units, half), lambda i, c: (1 - c[0], 0, 0)),
            ],
            out_specs=pl.BlockSpec((block, half), lambda i, c: (i, 0)),
        ),
        out_shape=jax.ShapeDtypeStruct((rows, half), BF16),
        cost_estimate=pl.CostEstimate(
            flops=4 * rows * half * units, bytes_accessed=2 * rows * (half + 2 * units), transcendentals=0
        ),
        name="down_rows",
    )(core, own, other, w_down, w_down)


def combine(ids, route, back, experts, first, count, before, last):
    tok = ids.shape[0]
    rows, half = back.shape
    block = block_of(rows, 512)
    steps = rows // block

    def kernel(ids_ref, route_ref, back_ref, *rest):
        before_ref = rest[0] if before is not None else None
        out_ref, place_ref, acc_ref = rest[-3:]
        step = pl.program_id(0)

        @pl.when(step == 0)
        def _():
            expert = lax.broadcasted_iota(jnp.int32, (tok, experts), 1)
            one = [ids_ref[:, k : k + 1] == expert for k in range(2)]
            named = jnp.where(one[0] | one[1], 1.0, 0.0).astype(BF16)
            slots = jnp.dot(strictly_before(tok, False), named, preferred_element_type=F32)
            for k in range(2):
                slot = jnp.sum(jnp.where(one[k], slots, 0.0), axis=1, keepdims=True).astype(jnp.int32) - first
                place = ids_ref[:, k : k + 1] * count + slot
                place = jnp.where((slot >= 0) & (slot < count), place, -1)
                place_ref[k] = jnp.broadcast_to(place, (tok, 128))
            if before is None:
                acc_ref[...] = jnp.zeros_like(acc_ref)
            else:
                acc_ref[...] = before_ref[...]

        lane = lax.broadcasted_iota(jnp.int32, (tok, block), 1) + step * block
        weight = jnp.where(place_ref[0, :, 0:1] == lane, route_ref[:, 0:1], 0.0)
        weight = jnp.where(place_ref[1, :, 0:1] == lane, route_ref[:, 1:2], weight)
        acc_ref[...] += jnp.dot(weight.astype(BF16), back_ref[...], preferred_element_type=F32)

        @pl.when(step == steps - 1)
        def _():
            out_ref[...] = acc_ref[...].astype(out_ref.dtype)

    whole = lambda i: (0, 0)
    operands = [ids, route, back]
    in_specs = [
        pl.BlockSpec((tok, 2), whole),
        pl.BlockSpec((tok, 2), whole),
        pl.BlockSpec((block, half), lambda i: (i, 0)),
    ]
    if before is not None:
        operands.append(before)
        in_specs.append(pl.BlockSpec((tok, half), whole))
    return pl.pallas_call(
        kernel,
        grid=(steps,),
        in_specs=in_specs,
        out_specs=pl.BlockSpec((tok, half), whole),
        out_shape=jax.ShapeDtypeStruct((tok, half), BF16 if last else F32),
        scratch_shapes=[pltpu.VMEM((2, tok, 128), jnp.int32), pltpu.VMEM((tok, half), F32)],
        cost_estimate=pl.CostEstimate(
            flops=2 * tok * rows * half, bytes_accessed=2 * (rows + tok) * half, transcendentals=0
        ),
        name="combine",
    )(*operands)


def on_device(tokens, norm_gain, expert_ids, route_weights, gate_weight, up_weight, down_weight):
    half = tokens.shape[1]
    experts = lax.axis_size("ep")
    core = lax.axis_index("tp").astype(jnp.int32).reshape(1)
    swap = [(0, 1), (1, 0)]
    ids_t = expert_ids.T
    w_gate, w_up, w_down = gate_weight[0], up_weight[0], down_weight[0]

    def exchange(array, count):
        array = array.reshape(experts, count, half)
        array = lax.all_to_all(array, "ep", split_axis=0, concat_axis=0, tiled=True)
        return array.reshape(experts * count, half)

    arrived = [
        exchange(select_rows(ids_t, tokens, experts, first, count), count) for first, count in CHUNKS
    ]
    returned = []
    for own, (first, count) in zip(arrived, CHUNKS):
        other = lax.ppermute(own, "tp", swap)
        hidden = hidden_units(core, own, other, norm_gain, w_gate, w_up)
        result = down_rows(core, hidden, lax.ppermute(hidden, "tp", swap), w_down)
        returned.append(exchange(result, count))
    total = None
    for n, (back, (first, count)) in enumerate(zip(returned, CHUNKS)):
        total = combine(expert_ids, route_weights, back, experts, first, count, total, n == len(CHUNKS) - 1)
    return total


def solution(mesh):
    in_specs = (
        P(("grp", "ep"), "tp"),
        P(),
        P(("grp", "ep"), None),
        P(("grp", "ep"), None),
        P("ep", None, "tp"),
        P("ep", None, "tp"),
        P("ep", None, "tp"),
    )
    out_specs = P(("grp", "ep"), "tp")
    return jax.shard_map(
        on_device, mesh=mesh, in_specs=in_specs, out_specs=out_specs, check_vma=False
    )
```

```python
import jax
import jax.numpy as jnp
from jax import lax
from jax.experimental import pallas as pl
from jax.experimental.pallas import tpu as pltpu
from jax.sharding import PartitionSpec as P

CAPACITY = 24
PIECES = 3
VMEM = 20 * 1024 * 1024
BF16 = jnp.bfloat16
F32 = jnp.float32
ANY = pl.BlockSpec(memory_space=pl.ANY)


def block_of(total, most):
    size = most
    while total % size:
        size -= 8
    return size


def slots_of(ids_ref, experts):
    tok = ids_ref.shape[1]
    expert = lax.broadcasted_iota(jnp.int32, (experts, tok), 0)
    one = [ids_ref[k : k + 1, :] == expert for k in range(2)]
    named = one[0] | one[1]
    row = lax.broadcasted_iota(jnp.int32, (tok, tok), 0)
    col = lax.broadcasted_iota(jnp.int32, (tok, tok), 1)
    before = jnp.where(row < col, 1.0, 0.0).astype(BF16)
    slot = jnp.dot(jnp.where(named, 1.0, 0.0).astype(BF16), before, preferred_element_type=F32)
    return one, named, slot


def select_rows(ids_t, tokens, experts):
    tok, half = tokens.shape
    per = block_of(experts, 16)

    def kernel(ids_ref, tok_ref, out_ref, key_ref):
        step = pl.program_id(0)

        @pl.when(step == 0)
        def _():
            _, named, slot = slots_of(ids_ref, experts)
            key_ref[...] = jnp.where(named, slot, -1.0)

        key = key_ref[pl.ds(pl.multiple_of(step * per, per), per), :]
        wanted = lax.broadcasted_iota(jnp.int32, (per, CAPACITY, tok), 1).astype(F32)
        chosen = jnp.where(key[:, None, :] == wanted, 1.0, 0.0).reshape(per * CAPACITY, tok).astype(BF16)
        out_ref[...] = jnp.dot(chosen, tok_ref[...], preferred_element_type=F32).astype(BF16)

    return pl.pallas_call(
        kernel,
        grid=(experts // per,),
        in_specs=[
            pl.BlockSpec((2, tok), lambda i: (0, 0)),
            pl.BlockSpec((tok, half), lambda i: (0, 0)),
        ],
        out_specs=pl.BlockSpec((per * CAPACITY, half), lambda i: (i, 0)),
        out_shape=jax.ShapeDtypeStruct((experts * CAPACITY, half), BF16),
        scratch_shapes=[pltpu.VMEM((experts, tok), F32)],
        cost_estimate=pl.CostEstimate(
            flops=2 * experts * CAPACITY * tok * half,
            bytes_accessed=2 * (tok + experts * CAPACITY) * half,
            transcendentals=0,
        ),
        compiler_params=pltpu.CompilerParams(vmem_limit_bytes=VMEM),
        name="select_rows",
    )(ids_t, tokens)


def combine_matrix(ids_t, route_t, experts, after):
    tok = ids_t.shape[1]
    rows = experts * CAPACITY

    def kernel(ids_ref, route_ref, after_ref, out_ref):
        one, _, slot = slots_of(ids_ref, experts)
        places = []
        for k in range(2):
            mine = jnp.sum(jnp.where(one[k], slot, 0.0), axis=0, keepdims=True)
            places.append(ids_ref[k : k + 1, :].astype(F32) * CAPACITY + mine)
        lines = jnp.concatenate(places + [route_ref[...], jnp.zeros((4, tok), F32)], axis=0).T
        lane = lax.broadcasted_iota(jnp.int32, (tok, rows), 1).astype(F32)
        weight = jnp.where(lines[:, 0:1] == lane, lines[:, 2:3], 0.0)
        out_ref[...] = jnp.where(lines[:, 1:2] == lane, lines[:, 3:4], weight).astype(BF16)

    return pl.pallas_call(
        kernel,
        in_specs=[
            pl.BlockSpec((2, tok), lambda: (0, 0)),
            pl.BlockSpec((2, tok), lambda: (0, 0)),
            ANY,
        ],
        out_specs=pl.BlockSpec((tok, rows), lambda: (0, 0)),
        out_shape=jax.ShapeDtypeStruct((tok, rows), BF16),
        cost_estimate=pl.CostEstimate(flops=4 * tok * rows, bytes_accessed=2 * tok * rows, transcendentals=0),
        compiler_params=pltpu.CompilerParams(vmem_limit_bytes=VMEM),
        name="combine_matrix",
    )(ids_t, route_t, after)


def hidden_units(core, own, other, first, gain, w_gate, w_up):
    rows, half = other.shape
    units = w_gate.shape[1]
    block = block_of(rows, 256)
    skip = first // block

    def kernel(core_ref, own_ref, other_ref, gain_a, gain_b, wg_a, wg_b, wu_a, wu_b, out_ref):
        a = own_ref[...].astype(F32)
        b = other_ref[...].astype(F32)
        total = jnp.sum(a * a, axis=-1, keepdims=True) + jnp.sum(b * b, axis=-1, keepdims=True)
        scale = lax.rsqrt(total * (1.0 / (2 * half)) + 1e-06)
        na = (a * scale * gain_a[0]).astype(BF16)
        nb = (b * scale * gain_b[0]).astype(BF16)
        gate = jnp.dot(na, wg_a[0], preferred_element_type=F32) + jnp.dot(nb, wg_b[0], preferred_element_type=F32)
        upper = jnp.dot(na, wu_a[0], preferred_element_type=F32) + jnp.dot(nb, wu_b[0], preferred_element_type=F32)
        out_ref[...] = (gate / (1.0 + jnp.exp(-gate)) * upper).astype(BF16)

    mine = lambda i, c: (c[0], 0, 0)
    theirs = lambda i, c: (1 - c[0], 0, 0)
    w_gate = w_gate.reshape(2, half, units)
    w_up = w_up.reshape(2, half, units)
    gain = gain.reshape(2, 1, half)
    return pl.pallas_call(
        kernel,
        grid_spec=pltpu.PrefetchScalarGridSpec(
            num_scalar_prefetch=1,
            grid=(rows // block,),
            in_specs=[
                pl.BlockSpec((block, half), lambda i, c: (i + skip, 0)),
                pl.BlockSpec((block, half), lambda i, c: (i, 0)),
                pl.BlockSpec((1, 1, half), mine),
                pl.BlockSpec((1, 1, half), theirs),
                pl.BlockSpec((1, half, units), mine),
                pl.BlockSpec((1, half, units), theirs),
                pl.BlockSpec((1, half, units), mine),
                pl.BlockSpec((1, half, units), theirs),
            ],
            out_specs=pl.BlockSpec((block, units), lambda i, c: (i, 0)),
        ),
        out_shape=jax.ShapeDtypeStruct((rows, units), BF16),
        cost_estimate=pl.CostEstimate(
            flops=8 * rows * half * units, bytes_accessed=4 * rows * half, transcendentals=rows * units
        ),
        compiler_params=pltpu.CompilerParams(vmem_limit_bytes=VMEM),
        name="hidden_units",
    )(core, own, other, gain, gain, w_gate, w_gate, w_up, w_up)


def down_rows(core, own, other, first, w_down, total, result, after):
    rows, units = own.shape
    half = w_down.shape[1]
    block = block_of(rows, 256)
    skip = first // block

    def kernel(core_ref, own_ref, other_ref, w_a, w_b, *rest):
        out = jnp.dot(own_ref[...], w_a[0], preferred_element_type=F32)
        out = out + jnp.dot(other_ref[...], w_b[0], preferred_element_type=F32)
        rest[-1][...] = out.astype(BF16)

    w_down = w_down.reshape(2, units, half)
    operands = [core, own, other, w_down, w_down]
    in_specs = [
        pl.BlockSpec((block, units), lambda i, c: (i, 0)),
        pl.BlockSpec((block, units), lambda i, c: (i, 0)),
        pl.BlockSpec((1, units, half), lambda i, c: (c[0], 0, 0)),
        pl.BlockSpec((1, units, half), lambda i, c: (1 - c[0], 0, 0)),
    ]
    aliases = {}
    if after is not None:
        operands.append(after)
        in_specs.append(ANY)
    if result is not None:
        aliases = {len(operands): 0}
        operands.append(result)
        in_specs.append(ANY)
    return pl.pallas_call(
        kernel,
        grid_spec=pltpu.PrefetchScalarGridSpec(
            num_scalar_prefetch=1,
            grid=(rows // block,),
            in_specs=in_specs,
            out_specs=pl.BlockSpec((block, half), lambda i, c: (i + skip, 0)),
        ),
        out_shape=jax.ShapeDtypeStruct((total, half), BF16),
        input_output_aliases=aliases,
        cost_estimate=pl.CostEstimate(
            flops=4 * rows * half * units, bytes_accessed=2 * rows * (half + 2 * units), transcendentals=0
        ),
        compiler_params=pltpu.CompilerParams(vmem_limit_bytes=VMEM),
        name="down_rows",
    )(*operands)


def combine(weights, back):
    tok, rows = weights.shape
    half = back.shape[1]
    block = 256

    def kernel(weights_ref, back_ref, out_ref):
        out_ref[...] = jnp.dot(weights_ref[...], back_ref[...], preferred_element_type=F32).astype(BF16)

    return pl.pallas_call(
        kernel,
        grid=(half // block,),
        in_specs=[
            pl.BlockSpec((tok, rows), lambda i: (0, 0)),
            pl.BlockSpec((rows, block), lambda i: (0, i)),
        ],
        out_specs=pl.BlockSpec((tok, block), lambda i: (0, i)),
        out_shape=jax.ShapeDtypeStruct((tok, half), BF16),
        cost_estimate=pl.CostEstimate(
            flops=2 * tok * rows * half, bytes_accessed=2 * (rows * (half + tok) + tok * half), transcendentals=0
        ),
        compiler_params=pltpu.CompilerParams(vmem_limit_bytes=VMEM),
        name="combine",
    )(weights, back)


def on_device(tokens, norm_gain, expert_ids, route_weights, gate_weight, up_weight, down_weight):
    half = tokens.shape[1]
    experts = lax.axis_size("ep")
    core = lax.axis_index("tp").astype(jnp.int32).reshape(1)
    swap = [(0, 1), (1, 0)]
    ids_t, route_t = expert_ids.T, route_weights.T
    w_gate, w_up, w_down = gate_weight[0], up_weight[0], down_weight[0]
    rows = experts * CAPACITY

    def exchange(array):
        array = array.reshape(experts, CAPACITY, half)
        array = lax.all_to_all(array, "ep", split_axis=0, concat_axis=0, tiled=True)
        return array.reshape(rows, half)

    own = exchange(select_rows(ids_t, tokens, experts))
    length = rows // PIECES
    starts = range(0, rows, length)
    others = [lax.ppermute(own[first : first + length], "tp", swap) for first in starts]
    weights = combine_matrix(ids_t, route_t, experts, own)
    hidden = [
        hidden_units(core, own, other, first, norm_gain, w_gate, w_up) for first, other in zip(starts, others)
    ]
    crossed = [lax.ppermute(piece, "tp", swap) for piece in hidden]
    result = None
    for first, mine, theirs in zip(starts, hidden, crossed):
        after = weights if result is None else None
        result = down_rows(core, mine, theirs, first, w_down, rows, result, after)
    return combine(weights, exchange(result))


def solution(mesh):
    in_specs = (
        P(("grp", "ep"), "tp"),
        P(),
        P(("grp", "ep"), None),
        P(("grp", "ep"), None),
        P("ep", None, "tp"),
        P("ep", None, "tp"),
        P("ep", None, "tp"),
    )
    out_specs = P(("grp", "ep"), "tp")
    return jax.shard_map(
        on_device, mesh=mesh, in_specs=in_specs, out_specs=out_specs, check_vma=False
    )
```

```python
import jax
import jax.numpy as jnp
from jax import lax
from jax.experimental import pallas as pl
from jax.experimental.pallas import tpu as pltpu
from jax.sharding import PartitionSpec as P

CAPACITY = 24
PIECES = 3
PARAMS = pltpu.CompilerParams(vmem_limit_bytes=20 * 1024 * 1024)
BF16 = jnp.bfloat16
F32 = jnp.float32
ANY = pl.BlockSpec(memory_space=pl.ANY)
SCALAR = pl.BlockSpec(memory_space=pltpu.SMEM)
ONCHIP = pl.BlockSpec(memory_space=pltpu.VMEM)


def block_of(total, most):
    size = most
    while total % size:
        size -= 8
    return size


def slots_of(ids_ref, experts):
    tok = ids_ref.shape[1]
    expert = lax.broadcasted_iota(jnp.int32, (experts, tok), 0)
    one = [ids_ref[k : k + 1, :] == expert for k in range(2)]
    named = one[0] | one[1]
    row = lax.broadcasted_iota(jnp.int32, (tok, tok), 0)
    col = lax.broadcasted_iota(jnp.int32, (tok, tok), 1)
    before = jnp.where(row < col, 1.0, 0.0).astype(BF16)
    slot = jnp.dot(jnp.where(named, 1.0, 0.0).astype(BF16), before, preferred_element_type=F32)
    return one, named, slot


def select_rows(core, ids_t, tokens, experts):
    tok, half = tokens.shape
    per = block_of(experts, 16)

    def kernel(core_ref, ids_ref, tok_ref, out_ref, key_ref):
        step = pl.program_id(0)

        @pl.when(step == 0)
        def _():
            _, named, slot = slots_of(ids_ref, experts)
            key_ref[...] = jnp.where(named, slot, -1.0)

        key = key_ref[pl.ds(pl.multiple_of(step * per, per), per), :]
        wanted = lax.broadcasted_iota(jnp.int32, (per, CAPACITY, tok), 1).astype(F32)
        chosen = jnp.where(key[:, None, :] == wanted, 1.0, 0.0).reshape(per * CAPACITY, tok).astype(BF16)
        out_ref[...] = jnp.dot(chosen, tok_ref[...], preferred_element_type=F32).astype(BF16)

    return pl.pallas_call(
        kernel,
        grid=(experts // per,),
        in_specs=[SCALAR, ONCHIP, ONCHIP],
        out_specs=pl.BlockSpec((per * CAPACITY, half), lambda i: (i, 0)),
        out_shape=jax.ShapeDtypeStruct((experts * CAPACITY, half), BF16),
        scratch_shapes=[pltpu.VMEM((experts, tok), F32)],
        cost_estimate=pl.CostEstimate(
            flops=2 * experts * CAPACITY * tok * half,
            bytes_accessed=2 * (tok + experts * CAPACITY) * half,
            transcendentals=0,
        ),
        compiler_params=PARAMS,
        name="select_rows",
    )(core, ids_t, tokens)


def combine_matrix(ids_t, route_t, experts, after):
    tok = ids_t.shape[1]
    rows = experts * CAPACITY

    def kernel(ids_ref, route_ref, after_ref, out_ref):
        one, _, slot = slots_of(ids_ref, experts)
        places = []
        for k in range(2):
            mine = jnp.sum(jnp.where(one[k], slot, 0.0), axis=0, keepdims=True)
            places.append(ids_ref[k : k + 1, :].astype(F32) * CAPACITY + mine)
        lines = jnp.concatenate(places + [route_ref[...], jnp.zeros((4, tok), F32)], axis=0).T
        lane = lax.broadcasted_iota(jnp.int32, (tok, rows), 1).astype(F32)
        weight = jnp.where(lines[:, 0:1] == lane, lines[:, 2:3], 0.0)
        out_ref[...] = jnp.where(lines[:, 1:2] == lane, lines[:, 3:4], weight).astype(BF16)

    return pl.pallas_call(
        kernel,
        in_specs=[
            pl.BlockSpec((2, tok), lambda: (0, 0)),
            pl.BlockSpec((2, tok), lambda: (0, 0)),
            ANY,
        ],
        out_specs=pl.BlockSpec((tok, rows), lambda: (0, 0)),
        out_shape=jax.ShapeDtypeStruct((tok, rows), BF16),
        cost_estimate=pl.CostEstimate(flops=4 * tok * rows, bytes_accessed=2 * tok * rows, transcendentals=0),
        compiler_params=PARAMS,
        name="combine_matrix",
    )(ids_t, route_t, after)


def hidden_units(core, own, other, gain, w_gate, w_up, first, length, after):
    half = other.shape[1]
    units = w_gate.shape[1]
    block = block_of(length, 256)

    def kernel(core_ref, own_ref, other_ref, gain_ref, gate_ref, up_ref, *rest):
        out_ref = rest[-1]
        mine = core_ref[0]
        theirs = 1 - mine
        for start in range(0, length, block):
            part = pl.ds(first + start, block)
            a = own_ref[part, :].astype(F32)
            b = other_ref[part, :].astype(F32)
            total = jnp.sum(a * a + b * b, axis=-1, keepdims=True)
            scale = lax.rsqrt(total * (1.0 / (2 * half)) + 1e-06)
            a = (a * scale * gain_ref[mine]).astype(BF16)
            b = (b * scale * gain_ref[theirs]).astype(BF16)
            gate = jnp.dot(a, gate_ref[mine], preferred_element_type=F32)
            gate = gate + jnp.dot(b, gate_ref[theirs], preferred_element_type=F32)
            upper = jnp.dot(a, up_ref[mine], preferred_element_type=F32)
            upper = upper + jnp.dot(b, up_ref[theirs], preferred_element_type=F32)
            out_ref[pl.ds(start, block), :] = (gate / (1.0 + jnp.exp(-gate)) * upper).astype(BF16)

    extra = [] if after is None else [after]
    return pl.pallas_call(
        kernel,
        in_specs=[SCALAR] + [ONCHIP] * 5 + [ANY] * len(extra),
        out_specs=ONCHIP,
        out_shape=jax.ShapeDtypeStruct((length, units), BF16),
        cost_estimate=pl.CostEstimate(
            flops=8 * length * half * units, bytes_accessed=4 * length * half, transcendentals=length * units
        ),
        compiler_params=PARAMS,
        name="hidden_units",
    )(core, own, other, gain.reshape(2, 1, half), w_gate.reshape(2, half, units), w_up.reshape(2, half, units), *extra)


def down_rows(core, own, other, first, w_down, total, result):
    rows, units = own.shape
    half = w_down.shape[1]
    block = block_of(rows, 256)
    skip = first // block

    def kernel(core_ref, own_ref, other_ref, w_a, w_b, *rest):
        out = jnp.dot(own_ref[...], w_a[0], preferred_element_type=F32)
        out = out + jnp.dot(other_ref[...], w_b[0], preferred_element_type=F32)
        rest[-1][...] = out.astype(BF16)

    w_down = w_down.reshape(2, units, half)
    operands = [core, own, other, w_down, w_down]
    in_specs = [
        pl.BlockSpec((block, units), lambda i, c: (i, 0)),
        pl.BlockSpec((block, units), lambda i, c: (i, 0)),
        pl.BlockSpec((1, units, half), lambda i, c: (c[0], 0, 0)),
        pl.BlockSpec((1, units, half), lambda i, c: (1 - c[0], 0, 0)),
    ]
    aliases = {}
    if result is not None:
        aliases = {len(operands): 0}
        operands.append(result)
        in_specs.append(ANY)
    return pl.pallas_call(
        kernel,
        grid_spec=pltpu.PrefetchScalarGridSpec(
            num_scalar_prefetch=1,
            grid=(rows // block,),
            in_specs=in_specs,
            out_specs=pl.BlockSpec((block, half), lambda i, c: (i + skip, 0)),
        ),
        out_shape=jax.ShapeDtypeStruct((total, half), BF16),
        input_output_aliases=aliases,
        cost_estimate=pl.CostEstimate(
            flops=4 * rows * half * units, bytes_accessed=2 * rows * (half + 2 * units), transcendentals=0
        ),
        compiler_params=PARAMS,
        name="down_rows",
    )(*operands)


def combine(weights, back):
    tok, rows = weights.shape
    half = back.shape[1]
    block = 256

    def kernel(weights_ref, back_ref, out_ref):
        cols = pl.ds(pl.multiple_of(pl.program_id(0) * block, block), block)
        out_ref[...] = jnp.dot(weights_ref[...], back_ref[:, cols], preferred_element_type=F32).astype(BF16)

    return pl.pallas_call(
        kernel,
        grid=(half // block,),
        in_specs=[
            ONCHIP,
            ONCHIP,
        ],
        out_specs=pl.BlockSpec((tok, block), lambda i: (0, i)),
        out_shape=jax.ShapeDtypeStruct((tok, half), BF16),
        cost_estimate=pl.CostEstimate(
            flops=2 * tok * rows * half, bytes_accessed=2 * (rows * (half + tok) + tok * half), transcendentals=0
        ),
        compiler_params=PARAMS,
        name="combine",
    )(weights, back)


def on_device(tokens, norm_gain, expert_ids, route_weights, gate_weight, up_weight, down_weight):
    half = tokens.shape[1]
    experts = lax.axis_size("ep")
    core = lax.axis_index("tp").astype(jnp.int32).reshape(1)
    swap = [(0, 1), (1, 0)]
    ids_t, route_t = expert_ids.T, route_weights.T
    w_gate, w_up, w_down = gate_weight[0], up_weight[0], down_weight[0]
    rows = experts * CAPACITY

    def exchange(array):
        array = array.reshape(experts, CAPACITY, half)
        array = lax.all_to_all(array, "ep", split_axis=0, concat_axis=0, tiled=True)
        return array.reshape(rows, half)

    own = exchange(select_rows(core, ids_t, tokens, experts))
    other = lax.ppermute(own, "tp", swap)
    weights = combine_matrix(ids_t, route_t, experts, own)
    length = rows // PIECES
    result = None
    starts = range(0, rows, length)
    hidden = [
        hidden_units(core, own, other, norm_gain, w_gate, w_up, first, length, weights if first == 0 else None)
        for first in starts
    ]
    crossed = [lax.ppermute(piece, "tp", swap) for piece in hidden]
    for first, mine, theirs in zip(starts, hidden, crossed):
        result = down_rows(core, mine, theirs, first, w_down, rows, result)
    return combine(weights, exchange(result))


def solution(mesh):
    in_specs = (
        P(("grp", "ep"), "tp"),
        P(),
        P(("grp", "ep"), None),
        P(("grp", "ep"), None),
        P("ep", None, "tp"),
        P("ep", None, "tp"),
        P("ep", None, "tp"),
    )
    out_specs = P(("grp", "ep"), "tp")
    return jax.shard_map(
        on_device, mesh=mesh, in_specs=in_specs, out_specs=out_specs, check_vma=False
    )
```

```python
import jax
import jax.numpy as jnp
from jax import lax
from jax.experimental import pallas as pl
from jax.experimental.pallas import tpu as pltpu
from jax.sharding import PartitionSpec as P

CAPACITY = 24
PIECES_OF = 6
PIECE_ENDS = (2, 4, 6)
PARAMS = pltpu.CompilerParams(vmem_limit_bytes=20 * 1024 * 1024)
BF16 = jnp.bfloat16
F32 = jnp.float32
ANY = pl.BlockSpec(memory_space=pl.ANY)
SCALAR = pl.BlockSpec(memory_space=pltpu.SMEM)
ONCHIP = pl.BlockSpec(memory_space=pltpu.VMEM)


def block_of(total, most):
    size = most
    while total % size:
        size -= 8
    return size


def slots_of(ids_ref, experts):
    tok = ids_ref.shape[1]
    expert = lax.broadcasted_iota(jnp.int32, (experts, tok), 0)
    one = [ids_ref[k : k + 1, :] == expert for k in range(2)]
    named = one[0] | one[1]
    row = lax.broadcasted_iota(jnp.int32, (tok, tok), 0)
    col = lax.broadcasted_iota(jnp.int32, (tok, tok), 1)
    before = jnp.where(row < col, 1.0, 0.0).astype(BF16)
    slot = jnp.dot(jnp.where(named, 1.0, 0.0).astype(BF16), before, preferred_element_type=F32)
    return one, named, slot


def select_rows(core, ids_t, tokens, experts):
    tok, half = tokens.shape
    per = block_of(experts, 16)

    def kernel(core_ref, ids_ref, tok_ref, out_ref, key_ref):
        step = pl.program_id(0)

        @pl.when(step == 0)
        def _():
            _, named, slot = slots_of(ids_ref, experts)
            key_ref[...] = jnp.where(named, slot, -1.0)

        key = key_ref[pl.ds(pl.multiple_of(step * per, per), per), :]
        wanted = lax.broadcasted_iota(jnp.int32, (per, CAPACITY, tok), 1).astype(F32)
        chosen = jnp.where(key[:, None, :] == wanted, 1.0, 0.0).reshape(per * CAPACITY, tok).astype(BF16)
        out_ref[...] = jnp.dot(chosen, tok_ref[...], preferred_element_type=F32).astype(BF16)

    return pl.pallas_call(
        kernel,
        grid=(experts // per,),
        in_specs=[SCALAR, ONCHIP, ONCHIP],
        out_specs=pl.BlockSpec((per * CAPACITY, half), lambda i: (i, 0)),
        out_shape=jax.ShapeDtypeStruct((experts * CAPACITY, half), BF16),
        scratch_shapes=[pltpu.VMEM((experts, tok), F32)],
        cost_estimate=pl.CostEstimate(
            flops=2 * experts * CAPACITY * tok * half,
            bytes_accessed=2 * (tok + experts * CAPACITY) * half,
            transcendentals=0,
        ),
        compiler_params=PARAMS,
        name="select_rows",
    )(core, ids_t, tokens)


def combine_matrix(ids_t, route_t, experts, after):
    tok = ids_t.shape[1]
    rows = experts * CAPACITY

    def kernel(ids_ref, route_ref, after_ref, out_ref):
        one, _, slot = slots_of(ids_ref, experts)
        places = []
        for k in range(2):
            mine = jnp.sum(jnp.where(one[k], slot, 0.0), axis=0, keepdims=True)
            places.append(ids_ref[k : k + 1, :].astype(F32) * CAPACITY + mine)
        lines = jnp.concatenate(places + [route_ref[...], jnp.zeros((4, tok), F32)], axis=0).T
        lane = lax.broadcasted_iota(jnp.int32, (tok, rows), 1).astype(F32)
        weight = jnp.where(lines[:, 0:1] == lane, lines[:, 2:3], 0.0)
        out_ref[...] = jnp.where(lines[:, 1:2] == lane, lines[:, 3:4], weight).astype(BF16)

    return pl.pallas_call(
        kernel,
        in_specs=[
            pl.BlockSpec((2, tok), lambda: (0, 0)),
            pl.BlockSpec((2, tok), lambda: (0, 0)),
            ANY,
        ],
        out_specs=pl.BlockSpec((tok, rows), lambda: (0, 0)),
        out_shape=jax.ShapeDtypeStruct((tok, rows), BF16),
        cost_estimate=pl.CostEstimate(flops=4 * tok * rows, bytes_accessed=2 * tok * rows, transcendentals=0),
        compiler_params=PARAMS,
        name="combine_matrix",
    )(ids_t, route_t, after)


def hidden_units(core, own, other, gain, w_gate, w_up, first, after):
    length, half = other.shape
    units = w_gate.shape[1]
    block = block_of(length, 256)

    def kernel(core_ref, own_ref, other_ref, gain_ref, gate_ref, up_ref, *rest):
        out_ref = rest[-1]
        mine = core_ref[0]
        theirs = 1 - mine
        for start in range(0, length, block):
            part = pl.ds(first + start, block)
            a = own_ref[part, :].astype(F32)
            b = other_ref[pl.ds(start, block), :].astype(F32)
            total = jnp.sum(a * a + b * b, axis=-1, keepdims=True)
            scale = lax.rsqrt(total * (1.0 / (2 * half)) + 1e-06)
            a = (a * scale * gain_ref[mine]).astype(BF16)
            b = (b * scale * gain_ref[theirs]).astype(BF16)
            gate = jnp.dot(a, gate_ref[mine], preferred_element_type=F32)
            gate = gate + jnp.dot(b, gate_ref[theirs], preferred_element_type=F32)
            upper = jnp.dot(a, up_ref[mine], preferred_element_type=F32)
            upper = upper + jnp.dot(b, up_ref[theirs], preferred_element_type=F32)
            out_ref[pl.ds(start, block), :] = (gate / (1.0 + jnp.exp(-gate)) * upper).astype(BF16)

    extra = [] if after is None else [after]
    return pl.pallas_call(
        kernel,
        in_specs=[SCALAR] + [ONCHIP] * 5 + [ANY] * len(extra),
        out_specs=ONCHIP,
        out_shape=jax.ShapeDtypeStruct((length, units), BF16),
        cost_estimate=pl.CostEstimate(
            flops=8 * length * half * units, bytes_accessed=4 * length * half, transcendentals=length * units
        ),
        compiler_params=PARAMS,
        name="hidden_units",
    )(core, own, other, gain.reshape(2, 1, half), w_gate.reshape(2, half, units), w_up.reshape(2, half, units), *extra)


def first_down_rows(core, own, other, starts, w_down, total):
    units = own[0].shape[1]
    half = w_down.shape[1]
    count = len(own)

    def kernel(core_ref, w_ref, *rest):
        out_ref = rest[-1]
        mine = core_ref[0]
        theirs = 1 - mine
        for n, first in enumerate(starts):
            length = own[n].shape[0]
            block = block_of(length, 256)
            for start in range(0, length, block):
                part = pl.ds(start, block)
                out = jnp.dot(rest[n][part, :], w_ref[mine], preferred_element_type=F32)
                out = out + jnp.dot(rest[count + n][part, :], w_ref[theirs], preferred_element_type=F32)
                out_ref[pl.ds(first + start, block), :] = out.astype(BF16)

    rows = sum(piece.shape[0] for piece in own)
    return pl.pallas_call(
        kernel,
        in_specs=[SCALAR] + [ONCHIP] * (1 + 2 * count),
        out_specs=ONCHIP,
        out_shape=jax.ShapeDtypeStruct((total, half), BF16),
        cost_estimate=pl.CostEstimate(
            flops=4 * rows * half * units, bytes_accessed=2 * rows * (half + 2 * units), transcendentals=0
        ),
        compiler_params=PARAMS,
        name="first_down_rows",
    )(core, w_down.reshape(2, units, half), *own, *other)


def last_down_rows(core, own, other, first, w_down, result):
    rows, units = own.shape
    total, half = result.shape
    block = block_of(rows, 256)
    skip = first // block

    def kernel(core_ref, own_ref, other_ref, w_ref, result_ref, out_ref):
        mine = core_ref[0]
        part = pl.ds(pl.multiple_of(pl.program_id(0) * block, block), block)
        out = jnp.dot(own_ref[part, :], w_ref[mine], preferred_element_type=F32)
        out = out + jnp.dot(other_ref[part, :], w_ref[1 - mine], preferred_element_type=F32)
        out_ref[...] = out.astype(BF16)

    return pl.pallas_call(
        kernel,
        grid=(rows // block,),
        in_specs=[SCALAR, ONCHIP, ONCHIP, ONCHIP, ANY],
        out_specs=pl.BlockSpec((block, half), lambda i: (i + skip, 0)),
        out_shape=jax.ShapeDtypeStruct((total, half), BF16),
        input_output_aliases={4: 0},
        cost_estimate=pl.CostEstimate(
            flops=4 * rows * half * units, bytes_accessed=2 * rows * (half + 2 * units), transcendentals=0
        ),
        compiler_params=PARAMS,
        name="last_down_rows",
    )(core, own, other, w_down.reshape(2, units, half), result)


def combine(weights, back):
    tok, rows = weights.shape
    half = back.shape[1]
    block = half // 2

    def kernel(weights_ref, back_ref, out_ref):
        cols = pl.ds(pl.multiple_of(pl.program_id(0) * block, block), block)
        out_ref[...] = jnp.dot(weights_ref[...], back_ref[:, cols], preferred_element_type=F32).astype(BF16)

    return pl.pallas_call(
        kernel,
        grid=(half // block,),
        in_specs=[
            ONCHIP,
            ONCHIP,
        ],
        out_specs=pl.BlockSpec((tok, block), lambda i: (0, i)),
        out_shape=jax.ShapeDtypeStruct((tok, half), BF16),
        cost_estimate=pl.CostEstimate(
            flops=2 * tok * rows * half, bytes_accessed=2 * (rows * (half + tok) + tok * half), transcendentals=0
        ),
        compiler_params=PARAMS,
        name="combine",
    )(weights, back)


def on_device(tokens, norm_gain, expert_ids, route_weights, gate_weight, up_weight, down_weight):
    half = tokens.shape[1]
    experts = lax.axis_size("ep")
    core = lax.axis_index("tp").astype(jnp.int32).reshape(1)
    swap = [(0, 1), (1, 0)]
    ids_t, route_t = expert_ids.T, route_weights.T
    w_gate, w_up, w_down = gate_weight[0], up_weight[0], down_weight[0]
    rows = experts * CAPACITY

    def exchange(array):
        array = array.reshape(experts, CAPACITY, half)
        array = lax.all_to_all(array, "ep", split_axis=0, concat_axis=0, tiled=True)
        return array.reshape(rows, half)

    own = exchange(select_rows(core, ids_t, tokens, experts))
    weights = combine_matrix(ids_t, route_t, experts, own)
    ends = [rows * n // PIECES_OF for n in PIECE_ENDS]
    starts = [0] + ends[:-1]
    others = [lax.ppermute(own[first:end], "tp", swap) for first, end in zip(starts, ends)]
    hidden = [
        hidden_units(core, own, other, norm_gain, w_gate, w_up, first, weights if first == 0 else None)
        for first, other in zip(starts, others)
    ]
    crossed = [lax.ppermute(piece, "tp", swap) for piece in hidden]
    result = first_down_rows(core, hidden[:-1], crossed[:-1], starts[:-1], w_down, rows)
    result = last_down_rows(core, hidden[-1], crossed[-1], starts[-1], w_down, result)
    return combine(weights, exchange(result))


def solution(mesh):
    in_specs = (
        P(("grp", "ep"), "tp"),
        P(),
        P(("grp", "ep"), None),
        P(("grp", "ep"), None),
        P("ep", None, "tp"),
        P("ep", None, "tp"),
        P("ep", None, "tp"),
    )
    out_specs = P(("grp", "ep"), "tp")
    return jax.shard_map(
        on_device, mesh=mesh, in_specs=in_specs, out_specs=out_specs, check_vma=False
    )
```

```python
import jax
import jax.numpy as jnp
from jax import lax
from jax.experimental import pallas as pl
from jax.experimental.pallas import tpu as pltpu
from jax.sharding import PartitionSpec as P

CAPACITY = 24
PIECES_OF = 6
PIECE_ENDS = (2, 4, 6)
PARAMS = pltpu.CompilerParams(vmem_limit_bytes=20 * 1024 * 1024)
BF16 = jnp.bfloat16
F32 = jnp.float32
ANY = pl.BlockSpec(memory_space=pl.ANY)
SCALAR = pl.BlockSpec(memory_space=pltpu.SMEM)
ONCHIP = pl.BlockSpec(memory_space=pltpu.VMEM)


def block_of(total, most):
    size = most
    while total % size:
        size -= 8
    return size


def slots_of(ids_ref, experts):
    tok = ids_ref.shape[1]
    expert = lax.broadcasted_iota(jnp.int32, (experts, tok), 0)
    one = [ids_ref[k : k + 1, :] == expert for k in range(2)]
    named = one[0] | one[1]
    row = lax.broadcasted_iota(jnp.int32, (tok, tok), 0)
    col = lax.broadcasted_iota(jnp.int32, (tok, tok), 1)
    before = jnp.where(row < col, 1.0, 0.0).astype(BF16)
    slot = jnp.dot(jnp.where(named, 1.0, 0.0).astype(BF16), before, preferred_element_type=F32)
    return one, named, slot


def select_rows(core, ids_t, tokens, experts):
    tok, half = tokens.shape
    per = block_of(experts, 16)

    def kernel(core_ref, ids_ref, tok_ref, out_ref):
        _, named, slot = slots_of(ids_ref, experts)
        keys = jnp.where(named, slot, -1.0)
        wanted = lax.broadcasted_iota(jnp.int32, (per, CAPACITY, tok), 1).astype(F32)
        for first in range(0, experts, per):
            key = keys[first : first + per]
            chosen = jnp.where(key[:, None, :] == wanted, 1.0, 0.0).reshape(per * CAPACITY, tok).astype(BF16)
            out_ref[pl.ds(first * CAPACITY, per * CAPACITY), :] = jnp.dot(
                chosen, tok_ref[...], preferred_element_type=F32
            ).astype(BF16)

    return pl.pallas_call(
        kernel,
        in_specs=[SCALAR, ONCHIP, ONCHIP],
        out_specs=ONCHIP,
        out_shape=jax.ShapeDtypeStruct((experts * CAPACITY, half), BF16),
        cost_estimate=pl.CostEstimate(
            flops=2 * experts * CAPACITY * tok * half,
            bytes_accessed=2 * (tok + experts * CAPACITY) * half,
            transcendentals=0,
        ),
        compiler_params=PARAMS,
        name="select_rows",
    )(core, ids_t, tokens)


def combine_matrix(ids_t, route_t, experts, after):
    tok = ids_t.shape[1]
    rows = experts * CAPACITY

    def kernel(ids_ref, route_ref, after_ref, out_ref):
        one, _, slot = slots_of(ids_ref, experts)
        places = []
        for k in range(2):
            mine = jnp.sum(jnp.where(one[k], slot, 0.0), axis=0, keepdims=True)
            places.append(ids_ref[k : k + 1, :].astype(F32) * CAPACITY + mine)
        lines = jnp.concatenate(places + [route_ref[...], jnp.zeros((4, tok), F32)], axis=0).T
        lane = lax.broadcasted_iota(jnp.int32, (tok, rows), 1).astype(F32)
        weight = jnp.where(lines[:, 0:1] == lane, lines[:, 2:3], 0.0)
        out_ref[...] = jnp.where(lines[:, 1:2] == lane, lines[:, 3:4], weight).astype(BF16)

    return pl.pallas_call(
        kernel,
        in_specs=[
            pl.BlockSpec((2, tok), lambda: (0, 0)),
            pl.BlockSpec((2, tok), lambda: (0, 0)),
            ANY,
        ],
        out_specs=pl.BlockSpec((tok, rows), lambda: (0, 0)),
        out_shape=jax.ShapeDtypeStruct((tok, rows), BF16),
        cost_estimate=pl.CostEstimate(flops=4 * tok * rows, bytes_accessed=2 * tok * rows, transcendentals=0),
        compiler_params=PARAMS,
        name="combine_matrix",
    )(ids_t, route_t, after)


def hidden_units(core, own, other, gain, w_gate, w_up, first, after):
    length, half = other.shape
    units = w_gate.shape[1]
    block = block_of(length, 256)

    def kernel(core_ref, own_ref, other_ref, gain_ref, gate_ref, up_ref, *rest):
        out_ref = rest[-1]
        mine = core_ref[0]
        theirs = 1 - mine
        for start in range(0, length, block):
            part = pl.ds(first + start, block)
            a = own_ref[part, :].astype(F32)
            b = other_ref[pl.ds(start, block), :].astype(F32)
            total = jnp.sum(a * a + b * b, axis=-1, keepdims=True)
            scale = lax.rsqrt(total * (1.0 / (2 * half)) + 1e-06)
            a = (a * scale * gain_ref[mine]).astype(BF16)
            b = (b * scale * gain_ref[theirs]).astype(BF16)
            gate = jnp.dot(a, gate_ref[mine], preferred_element_type=F32)
            gate = gate + jnp.dot(b, gate_ref[theirs], preferred_element_type=F32)
            upper = jnp.dot(a, up_ref[mine], preferred_element_type=F32)
            upper = upper + jnp.dot(b, up_ref[theirs], preferred_element_type=F32)
            out_ref[pl.ds(start, block), :] = (gate / (1.0 + jnp.exp(-gate)) * upper).astype(BF16)

    extra = [] if after is None else [after]
    return pl.pallas_call(
        kernel,
        in_specs=[SCALAR] + [ONCHIP] * 5 + [ANY] * len(extra),
        out_specs=ONCHIP,
        out_shape=jax.ShapeDtypeStruct((length, units), BF16),
        cost_estimate=pl.CostEstimate(
            flops=8 * length * half * units, bytes_accessed=4 * length * half, transcendentals=length * units
        ),
        compiler_params=PARAMS,
        name="hidden_units",
    )(core, own, other, gain.reshape(2, 1, half), w_gate.reshape(2, half, units), w_up.reshape(2, half, units), *extra)


def first_down_rows(core, own, other, starts, w_down, total):
    units = own[0].shape[1]
    half = w_down.shape[1]
    count = len(own)

    def kernel(core_ref, w_ref, *rest):
        out_ref = rest[-1]
        mine = core_ref[0]
        theirs = 1 - mine
        for n, first in enumerate(starts):
            length = own[n].shape[0]
            block = block_of(length, 256)
            for start in range(0, length, block):
                part = pl.ds(start, block)
                out = jnp.dot(rest[n][part, :], w_ref[mine], preferred_element_type=F32)
                out = out + jnp.dot(rest[count + n][part, :], w_ref[theirs], preferred_element_type=F32)
                out_ref[pl.ds(first + start, block), :] = out.astype(BF16)

    rows = sum(piece.shape[0] for piece in own)
    return pl.pallas_call(
        kernel,
        in_specs=[SCALAR] + [ONCHIP] * (1 + 2 * count),
        out_specs=ONCHIP,
        out_shape=jax.ShapeDtypeStruct((total, half), BF16),
        cost_estimate=pl.CostEstimate(
            flops=4 * rows * half * units, bytes_accessed=2 * rows * (half + 2 * units), transcendentals=0
        ),
        compiler_params=PARAMS,
        name="first_down_rows",
    )(core, w_down.reshape(2, units, half), *own, *other)


def last_down_rows(core, own, other, first, w_down, result):
    rows, units = own.shape
    total, half = result.shape
    block = block_of(rows, 256)
    skip = first // block

    def kernel(core_ref, own_ref, other_ref, w_ref, result_ref, out_ref):
        mine = core_ref[0]
        part = pl.ds(pl.multiple_of(pl.program_id(0) * block, block), block)
        out = jnp.dot(own_ref[part, :], w_ref[mine], preferred_element_type=F32)
        out = out + jnp.dot(other_ref[part, :], w_ref[1 - mine], preferred_element_type=F32)
        out_ref[...] = out.astype(BF16)

    return pl.pallas_call(
        kernel,
        grid=(rows // block,),
        in_specs=[SCALAR, ONCHIP, ONCHIP, ONCHIP, ANY],
        out_specs=pl.BlockSpec((block, half), lambda i: (i + skip, 0)),
        out_shape=jax.ShapeDtypeStruct((total, half), BF16),
        input_output_aliases={4: 0},
        cost_estimate=pl.CostEstimate(
            flops=4 * rows * half * units, bytes_accessed=2 * rows * (half + 2 * units), transcendentals=0
        ),
        compiler_params=PARAMS,
        name="last_down_rows",
    )(core, own, other, w_down.reshape(2, units, half), result)


def combine(weights, back):
    tok, rows = weights.shape
    half = back.shape[1]
    block = half // 2

    def kernel(weights_ref, back_ref, out_ref):
        cols = pl.ds(pl.multiple_of(pl.program_id(0) * block, block), block)
        out_ref[...] = jnp.dot(weights_ref[...], back_ref[:, cols], preferred_element_type=F32).astype(BF16)

    return pl.pallas_call(
        kernel,
        grid=(half // block,),
        in_specs=[
            ONCHIP,
            ONCHIP,
        ],
        out_specs=pl.BlockSpec((tok, block), lambda i: (0, i)),
        out_shape=jax.ShapeDtypeStruct((tok, half), BF16),
        cost_estimate=pl.CostEstimate(
            flops=2 * tok * rows * half, bytes_accessed=2 * (rows * (half + tok) + tok * half), transcendentals=0
        ),
        compiler_params=PARAMS,
        name="combine",
    )(weights, back)


def on_device(tokens, norm_gain, expert_ids, route_weights, gate_weight, up_weight, down_weight):
    half = tokens.shape[1]
    experts = lax.axis_size("ep")
    core = lax.axis_index("tp").astype(jnp.int32).reshape(1)
    swap = [(0, 1), (1, 0)]
    ids_t, route_t = expert_ids.T, route_weights.T
    w_gate, w_up, w_down = gate_weight[0], up_weight[0], down_weight[0]
    rows = experts * CAPACITY

    def exchange(array):
        array = array.reshape(experts, CAPACITY, half)
        array = lax.all_to_all(array, "ep", split_axis=0, concat_axis=0, tiled=True)
        return array.reshape(rows, half)

    own = exchange(select_rows(core, ids_t, tokens, experts))
    weights = combine_matrix(ids_t, route_t, experts, own)
    ends = [rows * n // PIECES_OF for n in PIECE_ENDS]
    starts = [0] + ends[:-1]
    others = [lax.ppermute(own[first:end], "tp", swap) for first, end in zip(starts, ends)]
    hidden = [
        hidden_units(core, own, other, norm_gain, w_gate, w_up, first, weights if first == 0 else None)
        for first, other in zip(starts, others)
    ]
    crossed = [lax.ppermute(piece, "tp", swap) for piece in hidden]
    result = first_down_rows(core, hidden[:-1], crossed[:-1], starts[:-1], w_down, rows)
    result = last_down_rows(core, hidden[-1], crossed[-1], starts[-1], w_down, result)
    return combine(weights, exchange(result))


def solution(mesh):
    in_specs = (
        P(("grp", "ep"), "tp"),
        P(),
        P(("grp", "ep"), None),
        P(("grp", "ep"), None),
        P("ep", None, "tp"),
        P("ep", None, "tp"),
        P("ep", None, "tp"),
    )
    out_specs = P(("grp", "ep"), "tp")
    return jax.shard_map(
        on_device, mesh=mesh, in_specs=in_specs, out_specs=out_specs, check_vma=False
    )
```

```python
import jax
import jax.numpy as jnp
from jax import lax
from jax.experimental import pallas as pl
from jax.experimental.pallas import tpu as pltpu
from jax.sharding import PartitionSpec as P

CAPACITY = 24
PIECES_OF = 6
PIECE_ENDS = (2, 4, 6)
PARAMS = pltpu.CompilerParams(vmem_limit_bytes=20 * 1024 * 1024)
BF16 = jnp.bfloat16
F32 = jnp.float32
ANY = pl.BlockSpec(memory_space=pl.ANY)
SCALAR = pl.BlockSpec(memory_space=pltpu.SMEM)
ONCHIP = pl.BlockSpec(memory_space=pltpu.VMEM)


def block_of(total, most):
    size = most
    while total % size:
        size -= 8
    return size


def slots_of(ids_ref, experts):
    tok = ids_ref.shape[1]
    expert = lax.broadcasted_iota(jnp.int32, (experts, tok), 0)
    one = [ids_ref[k : k + 1, :] == expert for k in range(2)]
    named = one[0] | one[1]
    row = lax.broadcasted_iota(jnp.int32, (tok, tok), 0)
    col = lax.broadcasted_iota(jnp.int32, (tok, tok), 1)
    before = jnp.where(row < col, 1.0, 0.0).astype(BF16)
    slot = jnp.dot(jnp.where(named, 1.0, 0.0).astype(BF16), before, preferred_element_type=F32)
    return one, named, slot


def select_rows(core, ids_t, tokens, experts):
    tok, half = tokens.shape
    per = block_of(experts, 16)

    def kernel(core_ref, ids_ref, tok_ref, out_ref):
        _, named, slot = slots_of(ids_ref, experts)
        keys = jnp.where(named, slot, -1.0)
        wanted = lax.broadcasted_iota(jnp.int32, (per, CAPACITY, tok), 1).astype(F32)
        for first in range(0, experts, per):
            key = keys[first : first + per]
            chosen = jnp.where(key[:, None, :] == wanted, 1.0, 0.0).reshape(per * CAPACITY, tok).astype(BF16)
            out_ref[pl.ds(first * CAPACITY, per * CAPACITY), :] = jnp.dot(
                chosen, tok_ref[...], preferred_element_type=F32
            ).astype(BF16)

    return pl.pallas_call(
        kernel,
        in_specs=[SCALAR, ONCHIP, ONCHIP],
        out_specs=ONCHIP,
        out_shape=jax.ShapeDtypeStruct((experts * CAPACITY, half), BF16),
        cost_estimate=pl.CostEstimate(
            flops=2 * experts * CAPACITY * tok * half,
            bytes_accessed=2 * (tok + experts * CAPACITY) * half,
            transcendentals=0,
        ),
        compiler_params=PARAMS,
        name="select_rows",
    )(core, ids_t, tokens)


def combine_matrix(ids_t, route_t, experts, after):
    tok = ids_t.shape[1]
    rows = experts * CAPACITY

    def kernel(ids_ref, route_ref, after_ref, out_ref):
        one, _, slot = slots_of(ids_ref, experts)
        places = []
        for k in range(2):
            mine = jnp.sum(jnp.where(one[k], slot, 0.0), axis=0, keepdims=True)
            places.append(ids_ref[k : k + 1, :].astype(F32) * CAPACITY + mine)
        lines = jnp.concatenate(places + [route_ref[...], jnp.zeros((4, tok), F32)], axis=0).T
        lane = lax.broadcasted_iota(jnp.int32, (tok, rows), 1).astype(F32)
        weight = jnp.where(lines[:, 0:1] == lane, lines[:, 2:3], 0.0)
        out_ref[...] = jnp.where(lines[:, 1:2] == lane, lines[:, 3:4], weight).astype(BF16)

    return pl.pallas_call(
        kernel,
        in_specs=[
            pl.BlockSpec((2, tok), lambda: (0, 0)),
            pl.BlockSpec((2, tok), lambda: (0, 0)),
            ANY,
        ],
        out_specs=pl.BlockSpec((tok, rows), lambda: (0, 0)),
        out_shape=jax.ShapeDtypeStruct((tok, rows), BF16),
        cost_estimate=pl.CostEstimate(flops=4 * tok * rows, bytes_accessed=2 * tok * rows, transcendentals=0),
        compiler_params=PARAMS,
        name="combine_matrix",
    )(ids_t, route_t, after)


def hidden_units(core, own, other, gain, w_gate, w_up, first, room, after, result):
    length, half = other.shape
    units = w_gate.shape[1]
    block = block_of(length, 256)

    def kernel(core_ref, own_ref, other_ref, gain_ref, gate_ref, up_ref, *rest):
        out_ref = rest[-1]
        mine = core_ref[0]
        theirs = 1 - mine
        for start in range(0, length, block):
            part = pl.ds(first + start, block)
            a = own_ref[part, :].astype(F32)
            b = other_ref[pl.ds(start, block), :].astype(F32)
            total = jnp.sum(a * a + b * b, axis=-1, keepdims=True)
            scale = lax.rsqrt(total * (1.0 / (2 * half)) + 1e-06)
            a = (a * scale * gain_ref[mine]).astype(BF16)
            b = (b * scale * gain_ref[theirs]).astype(BF16)
            gate = jnp.dot(a, gate_ref[mine], preferred_element_type=F32)
            gate = gate + jnp.dot(b, gate_ref[theirs], preferred_element_type=F32)
            upper = jnp.dot(a, up_ref[mine], preferred_element_type=F32)
            upper = upper + jnp.dot(b, up_ref[theirs], preferred_element_type=F32)
            out_ref[pl.ds(start, block), :] = (gate / (1.0 + jnp.exp(-gate)) * upper).astype(BF16)

    extra = [x for x in (after, result) if x is not None]
    aliases = {} if result is None else {5 + len(extra): 0}
    out_spec = ONCHIP if result is None else pl.BlockSpec((length, units), lambda i: (first // length, 0))
    return pl.pallas_call(
        kernel,
        grid=() if result is None else (1,),
        in_specs=[SCALAR] + [ONCHIP] * 5 + [ANY] * len(extra),
        out_specs=out_spec,
        out_shape=jax.ShapeDtypeStruct((room, units), BF16),
        input_output_aliases=aliases,
        cost_estimate=pl.CostEstimate(
            flops=8 * length * half * units, bytes_accessed=4 * length * half, transcendentals=length * units
        ),
        compiler_params=PARAMS,
        name="hidden_units",
    )(core, own, other, gain.reshape(2, 1, half), w_gate.reshape(2, half, units), w_up.reshape(2, half, units), *extra)


def first_down_rows(core, own, other, starts, w_down, total):
    units = own[0].shape[1]
    half = w_down.shape[1]
    count = len(own)

    def kernel(core_ref, w_ref, *rest):
        out_ref = rest[-1]
        mine = core_ref[0]
        theirs = 1 - mine
        for n, first in enumerate(starts):
            length = own[n].shape[0]
            block = block_of(length, 256)
            for start in range(0, length, block):
                part = pl.ds(start, block)
                out = jnp.dot(rest[n][part, :], w_ref[mine], preferred_element_type=F32)
                out = out + jnp.dot(rest[count + n][part, :], w_ref[theirs], preferred_element_type=F32)
                out_ref[pl.ds(first + start, block), :] = out.astype(BF16)

    rows = sum(piece.shape[0] for piece in own)
    return pl.pallas_call(
        kernel,
        in_specs=[SCALAR] + [ONCHIP] * (1 + 2 * count),
        out_specs=ONCHIP,
        out_shape=jax.ShapeDtypeStruct((total, half), BF16),
        cost_estimate=pl.CostEstimate(
            flops=4 * rows * half * units, bytes_accessed=2 * rows * (half + 2 * units), transcendentals=0
        ),
        compiler_params=PARAMS,
        name="first_down_rows",
    )(core, w_down.reshape(2, units, half), *own, *other)


def last_down_rows(core, own, other, first, w_down, result):
    rows, units = own.shape
    total, half = result.shape
    block = block_of(rows, 256)
    skip = first // block

    def kernel(core_ref, own_ref, other_ref, w_ref, result_ref, out_ref):
        mine = core_ref[0]
        part = pl.ds(pl.multiple_of(pl.program_id(0) * block, block), block)
        out = jnp.dot(own_ref[part, :], w_ref[mine], preferred_element_type=F32)
        out = out + jnp.dot(other_ref[part, :], w_ref[1 - mine], preferred_element_type=F32)
        out_ref[...] = out.astype(BF16)

    return pl.pallas_call(
        kernel,
        grid=(rows // block,),
        in_specs=[SCALAR, ONCHIP, ONCHIP, ONCHIP, ANY],
        out_specs=pl.BlockSpec((block, half), lambda i: (i + skip, 0)),
        out_shape=jax.ShapeDtypeStruct((total, half), BF16),
        input_output_aliases={4: 0},
        cost_estimate=pl.CostEstimate(
            flops=4 * rows * half * units, bytes_accessed=2 * rows * (half + 2 * units), transcendentals=0
        ),
        compiler_params=PARAMS,
        name="last_down_rows",
    )(core, own, other, w_down.reshape(2, units, half), result)


def combine(weights, back):
    tok, rows = weights.shape
    half = back.shape[1]
    block = 256

    def kernel(weights_ref, back_ref, out_hbm, out_ref, sems):
        copies = []
        for n in range(half // block):
            cols = pl.ds(n * block, block)
            out_ref[:, cols] = jnp.dot(weights_ref[...], back_ref[:, cols], preferred_element_type=F32).astype(BF16)
            copies.append(pltpu.make_async_copy(out_ref.at[:, cols], out_hbm.at[:, cols], sems.at[n]))
            copies[-1].start()
        for copy in copies:
            copy.wait()

    return pl.pallas_call(
        kernel,
        in_specs=[ONCHIP, ONCHIP],
        out_specs=ANY,
        out_shape=jax.ShapeDtypeStruct((tok, half), BF16),
        scratch_shapes=[pltpu.VMEM((tok, half), BF16), pltpu.SemaphoreType.DMA((half // block,))],
        cost_estimate=pl.CostEstimate(
            flops=2 * tok * rows * half, bytes_accessed=2 * (rows * (half + tok) + tok * half), transcendentals=0
        ),
        compiler_params=PARAMS,
        name="combine",
    )(weights, back)


def on_device(tokens, norm_gain, expert_ids, route_weights, gate_weight, up_weight, down_weight):
    half = tokens.shape[1]
    experts = lax.axis_size("ep")
    core = lax.axis_index("tp").astype(jnp.int32).reshape(1)
    swap = [(0, 1), (1, 0)]
    ids_t, route_t = expert_ids.T, route_weights.T
    w_gate, w_up, w_down = gate_weight[0], up_weight[0], down_weight[0]
    rows = experts * CAPACITY

    def exchange(array):
        array = array.reshape(experts, CAPACITY, half)
        array = lax.all_to_all(array, "ep", split_axis=0, concat_axis=0, tiled=True)
        return array.reshape(rows, half)

    own = exchange(select_rows(core, ids_t, tokens, experts))
    weights = combine_matrix(ids_t, route_t, experts, own)
    ends = [rows * n // PIECES_OF for n in PIECE_ENDS]
    starts = [0] + ends[:-1]
    others = [lax.ppermute(own[first:end], "tp", swap) for first, end in zip(starts, ends)]
    product = lambda n, room, after, result: hidden_units(
        core, own, others[n], norm_gain, w_gate, w_up, starts[n], room, after, result
    )
    early = product(1, ends[1], None, product(0, ends[1], weights, None))
    late = product(2, rows - ends[1], None, None)
    crossed = [lax.ppermute(piece, "tp", swap) for piece in (early, late)]
    result = first_down_rows(core, [early], crossed[:1], [0], w_down, rows)
    result = last_down_rows(core, late, crossed[1], ends[1], w_down, result)
    return combine(weights, exchange(result))


def solution(mesh):
    in_specs = (
        P(("grp", "ep"), "tp"),
        P(),
        P(("grp", "ep"), None),
        P(("grp", "ep"), None),
        P("ep", None, "tp"),
        P("ep", None, "tp"),
        P("ep", None, "tp"),
    )
    out_specs = P(("grp", "ep"), "tp")
    return jax.shard_map(
        on_device, mesh=mesh, in_specs=in_specs, out_specs=out_specs, check_vma=False
    )
```

```python
import jax
import jax.numpy as jnp
from jax import lax
from jax.experimental import pallas as pl
from jax.experimental.pallas import tpu as pltpu
from jax.sharding import PartitionSpec as P

CAPACITY = 24
PIECES_OF = 6
PIECE_ENDS = (2, 4, 6)
PARAMS = pltpu.CompilerParams(vmem_limit_bytes=20 * 1024 * 1024)
BF16 = jnp.bfloat16
F32 = jnp.float32
ANY = pl.BlockSpec(memory_space=pl.ANY)
SCALAR = pl.BlockSpec(memory_space=pltpu.SMEM)
ONCHIP = pl.BlockSpec(memory_space=pltpu.VMEM)


def block_of(total, most):
    size = most
    while total % size:
        size -= 8
    return size


def slots_of(ids_ref, experts):
    tok = ids_ref.shape[1]
    expert = lax.broadcasted_iota(jnp.int32, (experts, tok), 0)
    one = [ids_ref[k : k + 1, :] == expert for k in range(2)]
    named = one[0] | one[1]
    row = lax.broadcasted_iota(jnp.int32, (tok, tok), 0)
    col = lax.broadcasted_iota(jnp.int32, (tok, tok), 1)
    before = jnp.where(row < col, 1.0, 0.0).astype(BF16)
    slot = jnp.dot(jnp.where(named, 1.0, 0.0).astype(BF16), before, preferred_element_type=F32)
    return one, named, slot


def select_rows(core, ids_t, tokens, experts):
    tok, half = tokens.shape
    per = block_of(experts, 16)

    def kernel(core_ref, ids_ref, tok_ref, out_ref):
        _, named, slot = slots_of(ids_ref, experts)
        keys = jnp.where(named, slot, -1.0)
        wanted = lax.broadcasted_iota(jnp.int32, (per, CAPACITY, tok), 1).astype(F32)
        for first in range(0, experts, per):
            key = keys[first : first + per]
            chosen = jnp.where(key[:, None, :] == wanted, 1.0, 0.0).reshape(per * CAPACITY, tok).astype(BF16)
            out_ref[pl.ds(first * CAPACITY, per * CAPACITY), :] = jnp.dot(
                chosen, tok_ref[...], preferred_element_type=F32
            ).astype(BF16)

    return pl.pallas_call(
        kernel,
        in_specs=[SCALAR, ONCHIP, ONCHIP],
        out_specs=ONCHIP,
        out_shape=jax.ShapeDtypeStruct((experts * CAPACITY, half), BF16),
        cost_estimate=pl.CostEstimate(
            flops=2 * experts * CAPACITY * tok * half,
            bytes_accessed=2 * (tok + experts * CAPACITY) * half,
            transcendentals=0,
        ),
        compiler_params=PARAMS,
        name="select_rows",
    )(core, ids_t, tokens)


def combine_matrix(ids_t, route_t, experts, after):
    tok = ids_t.shape[1]
    rows = experts * CAPACITY

    def kernel(ids_ref, route_ref, after_ref, out_ref):
        one, _, slot = slots_of(ids_ref, experts)
        places = []
        for k in range(2):
            mine = jnp.sum(jnp.where(one[k], slot, 0.0), axis=0, keepdims=True)
            places.append(ids_ref[k : k + 1, :].astype(F32) * CAPACITY + mine)
        lines = jnp.concatenate(places + [route_ref[...], jnp.zeros((4, tok), F32)], axis=0).T
        lane = lax.broadcasted_iota(jnp.int32, (tok, rows), 1).astype(F32)
        weight = jnp.where(lines[:, 0:1] == lane, lines[:, 2:3], 0.0)
        out_ref[...] = jnp.where(lines[:, 1:2] == lane, lines[:, 3:4], weight).astype(BF16)

    return pl.pallas_call(
        kernel,
        in_specs=[
            pl.BlockSpec((2, tok), lambda: (0, 0)),
            pl.BlockSpec((2, tok), lambda: (0, 0)),
            ANY,
        ],
        out_specs=pl.BlockSpec((tok, rows), lambda: (0, 0)),
        out_shape=jax.ShapeDtypeStruct((tok, rows), BF16),
        cost_estimate=pl.CostEstimate(flops=4 * tok * rows, bytes_accessed=2 * tok * rows, transcendentals=0),
        compiler_params=PARAMS,
        name="combine_matrix",
    )(ids_t, route_t, after)


def hidden_units(core, own, other, gain, w_gate, w_up, first, room, after, result):
    length, half = other.shape
    units = w_gate.shape[1]
    block = block_of(length, 256)

    def kernel(core_ref, own_ref, other_ref, gain_ref, gate_ref, up_ref, *rest):
        out_ref = rest[-1]
        mine = core_ref[0]
        theirs = 1 - mine
        for start in range(0, length, block):
            part = pl.ds(first + start, block)
            a = own_ref[part, :].astype(F32)
            b = other_ref[pl.ds(start, block), :].astype(F32)
            total = jnp.sum(a * a + b * b, axis=-1, keepdims=True)
            scale = lax.rsqrt(total * (1.0 / (2 * half)) + 1e-06)
            a = (a * scale * gain_ref[mine]).astype(BF16)
            b = (b * scale * gain_ref[theirs]).astype(BF16)
            gate = jnp.dot(a, gate_ref[mine], preferred_element_type=F32)
            gate = gate + jnp.dot(b, gate_ref[theirs], preferred_element_type=F32)
            upper = jnp.dot(a, up_ref[mine], preferred_element_type=F32)
            upper = upper + jnp.dot(b, up_ref[theirs], preferred_element_type=F32)
            out_ref[pl.ds(start, block), :] = (gate / (1.0 + jnp.exp(-gate)) * upper).astype(BF16)

    extra = [x for x in (after, result) if x is not None]
    aliases = {} if result is None else {5 + len(extra): 0}
    out_spec = ONCHIP if result is None else pl.BlockSpec((length, units), lambda i: (first // length, 0))
    return pl.pallas_call(
        kernel,
        grid=() if result is None else (1,),
        in_specs=[SCALAR] + [ONCHIP] * 5 + [ANY] * len(extra),
        out_specs=out_spec,
        out_shape=jax.ShapeDtypeStruct((room, units), BF16),
        input_output_aliases=aliases,
        cost_estimate=pl.CostEstimate(
            flops=8 * length * half * units, bytes_accessed=4 * length * half, transcendentals=length * units
        ),
        compiler_params=PARAMS,
        name="hidden_units",
    )(core, own, other, gain.reshape(2, 1, half), w_gate.reshape(2, half, units), w_up.reshape(2, half, units), *extra)


def first_down_rows(core, own, other, starts, w_down, total):
    units = own[0].shape[1]
    half = w_down.shape[1]
    count = len(own)

    def kernel(core_ref, w_ref, *rest):
        out_ref = rest[-1]
        mine = core_ref[0]
        theirs = 1 - mine
        for n, first in enumerate(starts):
            length = own[n].shape[0]
            block = block_of(length, 256)
            for start in range(0, length, block):
                part = pl.ds(start, block)
                out = jnp.dot(rest[n][part, :], w_ref[mine], preferred_element_type=F32)
                out = out + jnp.dot(rest[count + n][part, :], w_ref[theirs], preferred_element_type=F32)
                out_ref[pl.ds(first + start, block), :] = out.astype(BF16)

    rows = sum(piece.shape[0] for piece in own)
    return pl.pallas_call(
        kernel,
        in_specs=[SCALAR] + [ONCHIP] * (1 + 2 * count),
        out_specs=ONCHIP,
        out_shape=jax.ShapeDtypeStruct((total, half), BF16),
        cost_estimate=pl.CostEstimate(
            flops=4 * rows * half * units, bytes_accessed=2 * rows * (half + 2 * units), transcendentals=0
        ),
        compiler_params=PARAMS,
        name="first_down_rows",
    )(core, w_down.reshape(2, units, half), *own, *other)


def last_down_rows(core, own, other, first, w_down, result):
    rows, units = own.shape
    total, half = result.shape
    block = block_of(rows, 256)

    def kernel(core_ref, own_ref, other_ref, w_ref, result_ref, out_ref):
        mine = core_ref[0]
        for start in range(0, rows, block):
            part = pl.ds(start, block)
            out = jnp.dot(own_ref[part, :], w_ref[mine], preferred_element_type=F32)
            out = out + jnp.dot(other_ref[part, :], w_ref[1 - mine], preferred_element_type=F32)
            out_ref[part, :] = out.astype(BF16)

    return pl.pallas_call(
        kernel,
        grid=(1,),
        in_specs=[SCALAR, ONCHIP, ONCHIP, ONCHIP, ANY],
        out_specs=pl.BlockSpec((rows, half), lambda i: (first // rows, 0)),
        out_shape=jax.ShapeDtypeStruct((total, half), BF16),
        input_output_aliases={4: 0},
        cost_estimate=pl.CostEstimate(
            flops=4 * rows * half * units, bytes_accessed=2 * rows * (half + 2 * units), transcendentals=0
        ),
        compiler_params=PARAMS,
        name="last_down_rows",
    )(core, own, other, w_down.reshape(2, units, half), result)


def combine(weights, back):
    tok, rows = weights.shape
    half = back.shape[1]
    block = 256

    def kernel(weights_ref, back_ref, out_hbm, out_ref, sems):
        copies = []
        for n in range(half // block):
            cols = pl.ds(n * block, block)
            out_ref[:, cols] = jnp.dot(weights_ref[...], back_ref[:, cols], preferred_element_type=F32).astype(BF16)
            copies.append(pltpu.make_async_copy(out_ref.at[:, cols], out_hbm.at[:, cols], sems.at[n]))
            copies[-1].start()
        for copy in copies:
            copy.wait()

    return pl.pallas_call(
        kernel,
        in_specs=[ONCHIP, ONCHIP],
        out_specs=ANY,
        out_shape=jax.ShapeDtypeStruct((tok, half), BF16),
        scratch_shapes=[pltpu.VMEM((tok, half), BF16), pltpu.SemaphoreType.DMA((half // block,))],
        cost_estimate=pl.CostEstimate(
            flops=2 * tok * rows * half, bytes_accessed=2 * (rows * (half + tok) + tok * half), transcendentals=0
        ),
        compiler_params=PARAMS,
        name="combine",
    )(weights, back)


def on_device(tokens, norm_gain, expert_ids, route_weights, gate_weight, up_weight, down_weight):
    half = tokens.shape[1]
    experts = lax.axis_size("ep")
    core = lax.axis_index("tp").astype(jnp.int32).reshape(1)
    swap = [(0, 1), (1, 0)]
    ids_t, route_t = expert_ids.T, route_weights.T
    w_gate, w_up, w_down = gate_weight[0], up_weight[0], down_weight[0]
    rows = experts * CAPACITY

    def exchange(array):
        array = array.reshape(experts, CAPACITY, half)
        array = lax.all_to_all(array, "ep", split_axis=0, concat_axis=0, tiled=True)
        return array.reshape(rows, half)

    own = exchange(select_rows(core, ids_t, tokens, experts))
    weights = combine_matrix(ids_t, route_t, experts, own)
    ends = [rows * n // PIECES_OF for n in PIECE_ENDS]
    starts = [0] + ends[:-1]
    others = [lax.ppermute(own[first:end], "tp", swap) for first, end in zip(starts, ends)]
    product = lambda n, room, after, result: hidden_units(
        core, own, others[n], norm_gain, w_gate, w_up, starts[n], room, after, result
    )
    early = product(1, ends[1], None, product(0, ends[1], weights, None))
    late = product(2, rows - ends[1], None, None)
    crossed = [lax.ppermute(piece, "tp", swap) for piece in (early, late)]
    result = first_down_rows(core, [early], crossed[:1], [0], w_down, rows)
    result = last_down_rows(core, late, crossed[1], ends[1], w_down, result)
    return combine(weights, exchange(result))


def solution(mesh):
    in_specs = (
        P(("grp", "ep"), "tp"),
        P(),
        P(("grp", "ep"), None),
        P(("grp", "ep"), None),
        P("ep", None, "tp"),
        P("ep", None, "tp"),
        P("ep", None, "tp"),
    )
    out_specs = P(("grp", "ep"), "tp")
    return jax.shard_map(
        on_device, mesh=mesh, in_specs=in_specs, out_specs=out_specs, check_vma=False
    )
```
